32 devices in a mesh: ep: 8 (over z, x), tp: 4 (over y, core).
Axes of the slice: x: 2, y: 2, z: 4, core: 2. Of those that a mesh axis runs over, the one named last changes fastest.
Arguments:
- mixer_input: bfloat16 [5120, 2048], P('ep'), may hold values from -6 to 6
- mixer_gain: float32 [2048], replicated, may hold values from 0.1 to 1.9
- value_weight: bfloat16 [2048, 1024], P(None, 'tp'), may hold values from -0.125 to 0.125
- inner_gate: bfloat16 [2048, 1024], P(None, 'tp'), may hold values from -0.125 to 0.125
- outer_gate: bfloat16 [2048, 1024], P(None, 'tp'), may hold values from -0.125 to 0.125
- kernel_taps: float32 [3, 1024], P(None, 'tp'), may hold values from -3 to 3
- mixer_proj: bfloat16 [1024, 2048], P('tp'), may hold values from -0.1875 to 0.1875
- expert_input: bfloat16 [5120, 2048], P(('ep', 'tp')), may hold values from -6 to 6
- expert_gain: float32 [2048], replicated, may hold values from 0.1 to 1.9
- routes: int32 [5120, 2], P(('ep', 'tp')), may hold values from 0 to 7, as said below
- group_logits: float32 [5120, 1], P(('ep', 'tp')), may hold values from -6 to 6
- pair_logits: float32 [5120, 2], P(('ep', 'tp')), may hold values from -6 to 6
- gate_weight: bfloat16 [8, 2048, 1024], P('ep', None, 'tp'), may hold values from -0.125 to 0.125
- up_weight: bfloat16 [8, 2048, 1024], P('ep', None, 'tp'), may hold values from -0.125 to 0.125
- down_weight: bfloat16 [8, 1024, 2048], P('ep', 'tp'), may hold values from -0.75 to 0.75
Outputs:
- mixer_output: bfloat16 [5120, 2048], P(('ep', 'tp'))
- expert_output: bfloat16 [5120, 2048], P(('ep', 'tp'))
The draws below stay inside these ranges and needn't reach their ends.
Inputs may be any that keep to these rules, and one draw needn't show every extreme that they name: `routes`: both entries of a row are different experts of one group (equal after integer division by 8). In the rows of one device every group is chosen by the same number of rows, no expert is named more than 80 times, and in every draw one expert is named exactly 80 times in the rows of every device.
All inputs are finite; a program needn't handle non-finite values.
Results may differ from the reference program's by a relative error of at most 0.01.
Values may be sent and summed in bfloat16 or wider, within the bound.
No kernel may reach another device: no remote copies, remote signals or barrier semaphores. Data moves between devices by JAX's collectives and lax.ppermute only.
A program may use at most 128 MiB of HBM per device.

```python
import jax
import jax.numpy as jnp
from jax import lax

D = 2048
CW = 1024
TAPS = 3
FF = 1024
EPG = 8
TOK_DEV = 160
GROUPS = 1
EXPERTS = 8
CAP = 80
TOKENS = 5120
N_EP = 8
N_TP = 4


def route_block(key, heavy, light):
    share = CAP // 2
    keys = jax.random.split(key, 4)
    group = jax.random.randint(keys[0], (), 0, GROUPS)
    order = jax.random.permutation(keys[1], EPG)
    raised = group * EPG + order[0]
    lowered = group * EPG + order[1]
    if share >= 2:
        shift = jax.random.randint(keys[2], (), 1, share)
    else:
        shift = jnp.zeros((), jnp.int32)
    clear = (raised != heavy) & (raised != light) & (lowered != heavy) & (lowered != light)
    shift = jnp.where(clear, shift, 0)
    experts_iota = jnp.arange(EXPERTS, dtype=jnp.int32)
    loads = (share + share * (experts_iota == heavy) - share * (experts_iota == light) + shift * (experts_iota == raised) - shift * (experts_iota == lowered)).astype(jnp.int32)
    bounds = jnp.cumsum(loads)
    per_group = EPG * share // 2
    place = jnp.arange(TOK_DEV, dtype=jnp.int32)
    first_slot = place // per_group * (2 * per_group) + place % per_group
    second_slot = first_slot + per_group
    first = jnp.sum((bounds[None, :] <= first_slot[:, None]).astype(jnp.int32), axis=1)
    second = jnp.sum((bounds[None, :] <= second_slot[:, None]).astype(jnp.int32), axis=1)
    pairs = jnp.stack([first, second], axis=1).astype(jnp.int32)
    shuffle = jax.random.permutation(keys[3], TOK_DEV)
    return jnp.zeros((TOK_DEV, 2), jnp.int32).at[shuffle].set(pairs)


def draw_routes(key, part):
    base = jax.random.fold_in(key, 17)
    picks = jax.random.split(jax.random.fold_in(base, 1), 2)
    group = jax.random.randint(picks[0], (), 0, GROUPS)
    order = jax.random.permutation(picks[1], EPG)
    heavy = group * EPG + order[0]
    light = group * EPG + order[1]
    block_keys = jax.random.split(jax.random.fold_in(base, 2), TOKENS // TOK_DEV)

    def one_block(block_key):
        return route_block(block_key, heavy, light)
    routed = jax.vmap(one_block)(block_keys)
    return routed.reshape(TOKENS, 2)


def level_of(key, dims, shards, smallest, largest):
    level = 1.0
    for position, shards_of in shards:
        steps = jax.random.uniform(jax.random.fold_in(jax.random.fold_in(key, 6), position), (shards_of,), jnp.float32, smallest / len(shards), largest / len(shards))
        level = level * jnp.repeat(jnp.exp(steps), dims[position] // shards_of).reshape((-1,) + (1,) * (len(dims) - 1 - position))
    return level


def normal_values(rng, extent, deviation, bound, cuts=(), kind=jnp.bfloat16):
    level = level_of(rng, extent, cuts, -0.22, 0.18) if cuts else 1.0
    drawn = jax.random.normal(rng, extent, jnp.float32) * deviation * level
    return jnp.minimum(jnp.maximum(drawn, -bound), bound).astype(kind)


def setup_inputs(seed: int = 0) -> dict:
    key_list = jax.random.split(jax.random.key(seed), 16)
    return {
        "mixer_input": normal_values(key_list[0], (TOKENS, D), 1.0, 6.0, ((0, 8),)),
        "mixer_gain": jnp.clip(1.0 + 0.18 * jax.random.normal(key_list[1], (D,), jnp.float32), 0.1, 1.9),
        "value_weight": normal_values(key_list[2], (D, CW), D ** -0.5, 0.125, ((1, 4),)),
        "inner_gate": normal_values(key_list[3], (D, CW), D ** -0.5, 0.125, ((1, 4),)),
        "outer_gate": normal_values(key_list[4], (D, CW), D ** -0.5, 0.125, ((1, 4),)),
        "kernel_taps": normal_values(key_list[5], (TAPS, CW), 0.6, 3.0, ((1, 4),), jnp.float32),
        "mixer_proj": normal_values(key_list[6], (CW, D), CW ** -0.5, 0.1875, ((0, 4),)),
        "expert_input": normal_values(key_list[7], (TOKENS, D), 1.0, 6.0, ((0, 32),)),
        "expert_gain": jnp.clip(1.0 + 0.18 * jax.random.normal(key_list[8], (D,), jnp.float32), 0.1, 1.9),
        "routes": draw_routes(jax.random.fold_in(key_list[15], 71), 0),
        "group_logits": normal_values(key_list[10], (TOKENS, GROUPS), 1.5, 6.0, ((0, 32),), jnp.float32),
        "pair_logits": normal_values(key_list[11], (TOKENS, 2), 1.5, 6.0, ((0, 32),), jnp.float32),
        "gate_weight": normal_values(key_list[12], (EXPERTS, D, FF), D ** -0.5, 0.125, ((0, 8), (2, 4))),
        "up_weight": normal_values(key_list[13], (EXPERTS, D, FF), D ** -0.5, 0.125, ((0, 8), (2, 4))),
        "down_weight": normal_values(key_list[14], (EXPERTS, FF, D), (FF // 16) ** -0.5, 0.75, ((0, 8), (1, 4))),
    }


EPSILON = 1e-06

def normed(values, gain):
    wide = values.astype(jnp.float32)
    scale = lax.rsqrt(lax.optimization_barrier(jnp.mean(wide * wide, axis=-1, keepdims=True)) + EPSILON)
    return (wide * scale * gain).astype(jnp.bfloat16)

def blockwise_sum(left, right, blocks):
    width = left.shape[1] // blocks
    total = jnp.zeros((left.shape[0], right.shape[1]), jnp.float32)
    for block in range(blocks):
        part = jnp.dot(left[:, block * width:(block + 1) * width], right[block * width:(block + 1) * width], preferred_element_type=jnp.float32)
        rounded = lax.optimization_barrier(part.astype(jnp.bfloat16))
        total = total + rounded.astype(jnp.float32)
    return total.astype(jnp.bfloat16)

def route_weights(routes, group_logits, pair_logits):
    chosen = routes[:, 0] // EPG
    groups = jnp.arange(group_logits.shape[1], dtype=jnp.int32)
    picked = lax.optimization_barrier(jnp.sum(jnp.where(groups[None, :] == chosen[:, None], group_logits, 0.0), axis=1))
    group_weight = 1.0 / lax.optimization_barrier(jnp.sum(jnp.exp(group_logits - picked[:, None]), axis=1))
    return group_weight[:, None] * jax.nn.sigmoid(pair_logits - pair_logits[:, ::-1])

def expert_block(rows, gate, upper, down, blocks):
    first = jnp.dot(rows, gate, preferred_element_type=jnp.float32)
    second = jnp.dot(rows, upper, preferred_element_type=jnp.float32)
    hidden = (jax.nn.silu(first) * second).astype(jnp.bfloat16)
    return blockwise_sum(hidden, down, blocks)

def reference(mixer_input, mixer_gain, value_weight, inner_gate, outer_gate, kernel_taps, mixer_proj, expert_input, expert_gain, routes, group_logits, pair_logits, gate_weight, up_weight, down_weight):
    normal_rows = normed(mixer_input, mixer_gain)
    values = jnp.dot(normal_rows, value_weight, preferred_element_type=jnp.float32)
    inner = jnp.dot(normal_rows, inner_gate, preferred_element_type=jnp.float32)
    outer = jnp.dot(normal_rows, outer_gate, preferred_element_type=jnp.float32)
    mixed_in = (inner * values).astype(jnp.bfloat16)
    padded = jnp.pad(mixed_in, ((1, 1), (0, 0))).astype(jnp.float32)
    conv_sum = kernel_taps[0] * padded[:-2] + kernel_taps[1] * padded[1:-1] + kernel_taps[2] * padded[2:]
    mixer_rows = (outer * conv_sum).astype(jnp.bfloat16)
    mixer_output = blockwise_sum(mixer_rows, mixer_proj, N_TP)
    expert_norm = normed(expert_input, expert_gain)
    weights = route_weights(routes, group_logits, pair_logits)
    flat = routes.reshape(-1)
    count = flat.shape[0]
    order = jnp.argsort(flat, stable=True).astype(jnp.int32)
    experts_iota = jnp.arange(EXPERTS, dtype=jnp.int32)
    loads = lax.optimization_barrier(jnp.sum((flat[:, None] == experts_iota[None, :]).astype(jnp.int32), axis=0))
    starts = (jnp.cumsum(loads) - loads).astype(jnp.int32)
    most = N_EP * N_TP * CAP
    padded_order = jnp.concatenate([order, jnp.full((most,), count, jnp.int32)])
    rows_pad = jnp.concatenate([expert_norm, jnp.zeros((1, D), jnp.bfloat16)])

    def one_expert(results, expert):
        picks = lax.dynamic_slice_in_dim(padded_order, starts[expert], most)
        live = jnp.arange(most, dtype=jnp.int32) < loads[expert]
        picks = jnp.where(live, picks, count).astype(jnp.int32)
        sources = jnp.where(live, picks // 2, count // 2).astype(jnp.int32)
        answers = expert_block(rows_pad[sources], gate_weight[expert], up_weight[expert], down_weight[expert], N_TP)
        return (results.at[picks].set(answers), None)
    results = jnp.zeros((count + 1, D), jnp.bfloat16)
    results, _ = lax.scan(one_expert, results, experts_iota)
    pairs = results[:count].reshape(count // 2, 2, D).astype(jnp.float32)
    expert_output = lax.optimization_barrier(jnp.sum(weights[:, :, None] * pairs, axis=1)).astype(jnp.bfloat16)
    return (mixer_output, expert_output)
```

```python
import jax
import jax.numpy as jnp
from jax import lax
from jax.experimental import pallas as pl
from jax.experimental.pallas import tpu as pltpu
from jax.sharding import PartitionSpec as P

EPG = 8
EPSILON = 1e-06
COLUMN_CHUNKS = 2


def padded_2(cells, sides, width):
    for axis, dim in sides:
        count = lax.axis_size(axis)
        ends = count - 1
        head = lax.slice_in_dim(cells, 0, width, axis=dim)
        tail = lax.slice_in_dim(cells, cells.shape[dim] - width, cells.shape[dim], axis=dim)
        cells = jnp.concatenate(
            [
                lax.ppermute(tail, axis, [(i, (i + 1) % count) for i in range(ends)]),
                cells,
                lax.ppermute(head, axis, [((i + 1) % count, i) for i in range(ends)]),
            ],
            axis=dim,
        )
    return cells


def normed(values, gain):
    wide = values.astype(jnp.float32)
    scale = lax.rsqrt(jnp.mean(wide * wide, axis=-1, keepdims=True) + EPSILON)
    return (wide * scale * gain).astype(jnp.bfloat16)


def swapped(value, axis, bit):
    count = lax.axis_size(axis)
    return lax.ppermute(value, axis, [(i, i ^ bit) for i in range(count)])


def dispatch_kernel(experts, capacity, me_ref, rows_ref, gain_ref, routes_ref, group_ref, pair_ref, *outs):
    hi_ref, lo_ref = outs[-2:]
    blocks = outs[:-2]
    wide = rows_ref[...].astype(jnp.float32)
    scale = lax.rsqrt(jnp.mean(wide * wide, axis=-1, keepdims=True) + EPSILON)
    norm = (wide * scale * gain_ref[...]).astype(jnp.bfloat16)
    local = norm.shape[0]
    first, second = routes_ref[0:1, :], routes_ref[1:2, :]
    expert = lax.broadcasted_iota(jnp.int32, (experts, local), 0)
    hit_first = jnp.where(expert == first, 1.0, 0.0)
    hit_second = jnp.where(expert == second, 1.0, 0.0)
    earlier = jnp.where(
        lax.broadcasted_iota(jnp.int32, (local, local), 0) < lax.broadcasted_iota(jnp.int32, (local, local), 1),
        1.0,
        0.0,
    ).astype(jnp.bfloat16)
    before_first = jnp.dot(hit_first.astype(jnp.bfloat16), earlier, preferred_element_type=jnp.float32)
    before_second = jnp.dot(hit_second.astype(jnp.bfloat16), earlier, preferred_element_type=jnp.float32)
    before_second = before_second + jnp.sum(hit_first, axis=1, keepdims=True)
    rank_first = jnp.sum(hit_first * before_first, axis=0, keepdims=True).astype(jnp.int32)
    rank_second = jnp.sum(hit_second * before_second, axis=0, keepdims=True).astype(jnp.int32)
    me = me_ref[0]
    slot_first = (first ^ me) * capacity + rank_first
    slot_second = (second ^ me) * capacity + rank_second
    slot = lax.broadcasted_iota(jnp.int32, (experts * capacity, local), 0)
    is_first = slot == slot_first
    is_second = slot == slot_second
    place = jnp.where(is_first | is_second, 1.0, 0.0).astype(jnp.bfloat16)
    placed = jnp.dot(place, norm, preferred_element_type=jnp.float32).astype(jnp.bfloat16)
    height = placed.shape[0] // len(blocks)
    for i, block in enumerate(blocks):
        block[...] = placed[i * height : (i + 1) * height]
    logits = group_ref[...]
    group = lax.broadcasted_iota(jnp.int32, logits.shape, 0)
    chosen = (group * EPG <= first) & (first < group * EPG + EPG)
    picked = jnp.sum(jnp.where(chosen, logits, 0.0), axis=0, keepdims=True)
    group_weight = 1.0 / jnp.sum(jnp.exp(logits - picked), axis=0, keepdims=True)
    apart = pair_ref[0:1, :] - pair_ref[1:2, :]
    weight_first = group_weight / (1.0 + jnp.exp(-apart))
    weight_second = group_weight / (1.0 + jnp.exp(apart))
    weights = jnp.where(is_first, weight_first, 0.0) + jnp.where(is_second, weight_second, 0.0)
    high = weights.astype(jnp.bfloat16)
    hi_ref[...] = high
    lo_ref[...] = (weights - high.astype(jnp.float32)).astype(jnp.bfloat16)


def combine_kernel(chunks, hi_ref, lo_ref, *refs):
    out_ref = refs[-1]
    answers = refs[:-1]
    per = len(answers) // chunks
    width = out_ref.shape[1] // chunks
    contract = (((0,), (0,)), ((), ()))
    for c in range(chunks):
        rows = jnp.concatenate([r[...] for r in answers[c * per : (c + 1) * per]], axis=0)
        total = lax.dot_general(hi_ref[...], rows, contract, preferred_element_type=jnp.float32)
        total = total + lax.dot_general(lo_ref[...], rows, contract, preferred_element_type=jnp.float32)
        out_ref[:, c * width : (c + 1) * width] = total.astype(jnp.bfloat16)


def gathered_blocks(piece, axis):
    count = lax.axis_size(axis)
    blocks = [piece]
    for k in range(1, count):
        low = k & -k
        blocks.append(swapped(blocks[k ^ low], axis, low))
    return blocks


def on_device(
    mixer_input,
    mixer_gain,
    value_weight,
    inner_gate,
    outer_gate,
    kernel_taps,
    mixer_proj,
    expert_input,
    expert_gain,
    routes,
    group_logits,
    pair_logits,
    gate_weight,
    up_weight,
    down_weight,
):
    experts = lax.axis_size("ep")
    split = lax.axis_size("tp")
    local, width = expert_input.shape
    capacity = 4 * local // experts
    direct = experts <= 8
    me_ep = lax.axis_index("ep").astype(jnp.int32)
    me_tp = lax.axis_index("tp").astype(jnp.int32)

    gates = gathered_blocks(gate_weight[0], "tp")
    uppers = gathered_blocks(up_weight[0], "tp")
    column = width // COLUMN_CHUNKS
    downs = [
        gathered_blocks(down_weight[0][:, c * column : (c + 1) * column], "tp") for c in range(COLUMN_CHUNKS)
    ]

    slots = experts * capacity
    height = capacity if direct else slots
    block = jax.ShapeDtypeStruct((height, width), jnp.bfloat16)
    share = jax.ShapeDtypeStruct((slots, local), jnp.bfloat16)
    vmem = pl.BlockSpec(memory_space=pltpu.VMEM)
    count = slots // height
    *outgoing, high, low = pl.pallas_call(
        lambda *refs: dispatch_kernel(experts, capacity, *refs),
        out_shape=[block] * count + [share, share],
        in_specs=[pl.BlockSpec(memory_space=pltpu.SMEM)] + [vmem] * 5,
        out_specs=[vmem] * (count + 2),
        name="dispatch",
    )(
        (me_ep if direct else jnp.zeros((), jnp.int32)).reshape(1),
        expert_input,
        expert_gain.reshape(1, width),
        routes.T,
        group_logits.T,
        pair_logits.T,
    )

    if direct:
        arrived = [outgoing[0]] + [None] * (experts - 1)
        for d in reversed(range(1, experts)):
            arrived[d] = swapped(outgoing[d], "ep", d)
        half = experts // 2
        groups = [(jnp.concatenate(arrived[half:]), half), (jnp.concatenate(arrived[:half]), 0)]
    else:
        whole = lax.all_to_all(
            outgoing[0].reshape(experts, capacity, width), "ep", split_axis=0, concat_axis=0, tiled=True
        )
        groups = [(whole.reshape(slots, width), 0)]

    normal_rows = normed(mixer_input, mixer_gain)
    values = jnp.dot(normal_rows, value_weight, preferred_element_type=jnp.float32)
    inner = jnp.dot(normal_rows, inner_gate, preferred_element_type=jnp.float32)
    outer = jnp.dot(normal_rows, outer_gate, preferred_element_type=jnp.float32)
    mixed_in = (inner * values).astype(jnp.bfloat16)
    padded = padded_2(mixed_in, (("ep", 0),), 1).astype(jnp.float32)
    conv_sum = (
        kernel_taps[0] * padded[:-2] + kernel_taps[1] * padded[1:-1] + kernel_taps[2] * padded[2:]
    )
    mixer_rows = (outer * conv_sum).astype(jnp.bfloat16)
    owned = mixer_rows.shape[0] // split
    parts = []
    for k in range(split):
        mine = lax.dynamic_slice_in_dim(mixer_rows, (me_tp ^ k) * owned, owned, axis=0)
        parts.append(jnp.dot(mine, mixer_proj, preferred_element_type=jnp.float32))
    bit = 1
    while bit < split:
        for k in range(0, split, 2 * bit):
            other = swapped(parts[k + bit].astype(jnp.bfloat16), "tp", bit)
            parts[k] = parts[k] + other.astype(jnp.float32)
        bit *= 2
    mixer_output = parts[0].astype(jnp.bfloat16)

    answered = [[None] * count for _ in range(COLUMN_CHUNKS)]
    for rows, start in groups:
        hidden = []
        for gate, upper in zip(gates, uppers):
            first = jnp.dot(rows, gate, preferred_element_type=jnp.float32)
            second = jnp.dot(rows, upper, preferred_element_type=jnp.float32)
            hidden.append((jax.nn.silu(first) * second).astype(jnp.bfloat16))
        for c in range(COLUMN_CHUNKS):
            total = sum(jnp.dot(h, w, preferred_element_type=jnp.float32) for h, w in zip(hidden, downs[c]))
            answer = total.astype(jnp.bfloat16)
            if direct:
                pieces = answer.shape[0] // capacity
                for p in reversed(range(pieces)):
                    d = start + p
                    piece = answer[p * capacity : (p + 1) * capacity]
                    answered[c][d] = swapped(piece, "ep", d) if d else piece
            else:
                back = lax.all_to_all(
                    answer.reshape(experts, capacity, column), "ep", split_axis=0, concat_axis=0, tiled=True
                )
                answered[c][0] = back.reshape(slots, column)

    flat = [a for chunk in answered for a in chunk]
    expert_output = pl.pallas_call(
        lambda *refs: combine_kernel(COLUMN_CHUNKS, *refs),
        out_shape=jax.ShapeDtypeStruct((local, width), jnp.bfloat16),
        in_specs=[vmem] * (2 + len(flat)),
        out_specs=vmem,
        name="combine",
    )(high, low, *flat)
    return (mixer_output, expert_output)


def solution(mesh):
    in_specs = (
        P("ep", None),
        P(),
        P(None, "tp"),
        P(None, "tp"),
        P(None, "tp"),
        P(None, "tp"),
        P("tp", None),
        P(("ep", "tp"), None),
        P(),
        P(("ep", "tp"), None),
        P(("ep", "tp"), None),
        P(("ep", "tp"), None),
        P("ep", None, "tp"),
        P("ep", None, "tp"),
        P("ep", "tp", None),
    )
    out_specs = (P(("ep", "tp"), None), P(("ep", "tp"), None))
    return jax.shard_map(
        on_device, mesh=mesh, in_specs=in_specs, out_specs=out_specs, check_vma=False
    )
```

```python
import jax
import jax.numpy as jnp
from jax import lax
from jax.experimental import pallas as pl
from jax.experimental.pallas import tpu as pltpu
from jax.sharding import PartitionSpec as P


EPG = 8
EPSILON = 1e-06


def swapped(value, axis, bit):
    count = lax.axis_size(axis)
    return lax.ppermute(value, axis, [(i, i ^ bit) for i in range(count)])


def call(body, outs, *operands, scratch=(), smem=0, aliases=None):
    vmem = pl.BlockSpec(memory_space=pltpu.VMEM)
    scalar = pl.BlockSpec(memory_space=pltpu.SMEM)
    single = not isinstance(outs, (list, tuple))
    return pl.pallas_call(
        body,
        out_shape=outs if single else list(outs),
        in_specs=[scalar] * smem + [vmem] * (len(operands) - smem),
        out_specs=vmem if single else [vmem] * len(outs),
        scratch_shapes=list(scratch),
        input_output_aliases=aliases or {},
    )(*operands)


def slots_of(experts, capacity, me, routes_ref):
    first, second = routes_ref[0:1, :], routes_ref[1:2, :]
    local = first.shape[1]
    expert = lax.broadcasted_iota(jnp.int32, (experts, local), 0)
    hit_first = jnp.where(expert == first, 1.0, 0.0)
    hit_second = jnp.where(expert == second, 1.0, 0.0)
    row = lax.broadcasted_iota(jnp.int32, (local, local), 0)
    column = lax.broadcasted_iota(jnp.int32, (local, local), 1)
    earlier = jnp.where(row < column, 1.0, 0.0).astype(jnp.bfloat16)
    before_first = jnp.dot(hit_first.astype(jnp.bfloat16), earlier, preferred_element_type=jnp.float32)
    before_second = jnp.dot(hit_second.astype(jnp.bfloat16), earlier, preferred_element_type=jnp.float32)
    before_second = before_second + jnp.sum(hit_first, axis=1, keepdims=True)
    rank_first = jnp.sum(hit_first * before_first, axis=0, keepdims=True).astype(jnp.int32)
    rank_second = jnp.sum(hit_second * before_second, axis=0, keepdims=True).astype(jnp.int32)
    slot = lax.broadcasted_iota(jnp.int32, (experts * capacity, local), 0)
    is_first = slot == (first ^ me) * capacity + rank_first
    is_second = slot == (second ^ me) * capacity + rank_second
    return is_first, is_second


def dispatch_kernel(experts, capacity, me_ref, rows_ref, gain_ref, routes_ref, *blocks):
    is_first, is_second = slots_of(experts, capacity, me_ref[0], routes_ref)
    place = jnp.where(is_first | is_second, 1.0, 0.0).astype(jnp.bfloat16)
    wide = rows_ref[...].astype(jnp.float32)
    scale = lax.rsqrt(jnp.mean(wide * wide, axis=-1, keepdims=True) + EPSILON)
    norm = (wide * scale * gain_ref[...]).astype(jnp.bfloat16)
    placed = jnp.dot(place, norm, preferred_element_type=jnp.float32).astype(jnp.bfloat16)
    height = placed.shape[0] // len(blocks)
    for i, block in enumerate(blocks):
        block[...] = placed[i * height : (i + 1) * height]


def share_kernel(experts, capacity, heights, me_ref, routes_ref, group_ref, pair_ref, *outs):
    is_first, is_second = slots_of(experts, capacity, me_ref[0], routes_ref)
    logits = group_ref[...]
    first = routes_ref[0:1, :]
    group = lax.broadcasted_iota(jnp.int32, logits.shape, 0)
    chosen = (group * EPG <= first) & (first < group * EPG + EPG)
    picked = jnp.sum(jnp.where(chosen, logits, 0.0), axis=0, keepdims=True)
    group_weight = 1.0 / jnp.sum(jnp.exp(logits - picked), axis=0, keepdims=True)
    apart = pair_ref[0:1, :] - pair_ref[1:2, :]
    weight_first = group_weight / (1.0 + jnp.exp(-apart))
    weight_second = group_weight / (1.0 + jnp.exp(apart))
    weights = jnp.where(is_first, weight_first, 0.0) + jnp.where(is_second, weight_second, 0.0)
    start = 0
    for i, height in enumerate(heights):
        share = weights[start : start + height].T
        high = share.astype(jnp.bfloat16)
        outs[2 * i][...] = high
        outs[2 * i + 1][...] = (share - high.astype(jnp.float32)).astype(jnp.bfloat16)
        start += height


def hidden_kernel(blocks, split, *refs):
    out_ref = refs[-1]
    rows = jnp.concatenate([r[...] for r in refs[:blocks]], axis=0)
    gates = refs[blocks : blocks + split]
    uppers = refs[blocks + split : blocks + 2 * split]
    width = gates[0].shape[1]
    for k in range(split):
        first = jnp.dot(rows, gates[k][...], preferred_element_type=jnp.float32)
        second = jnp.dot(rows, uppers[k][...], preferred_element_type=jnp.float32)
        value = first / (1.0 + jnp.exp(-first)) * second
        out_ref[:, k * width : (k + 1) * width] = value.astype(jnp.bfloat16)


def down_kernel(split, *refs):
    hidden_ref = refs[0]
    downs = refs[1 : 1 + split]
    outs = refs[1 + split :]
    width = downs[0].shape[0]
    total = None
    for k in range(split):
        part = jnp.dot(
            hidden_ref[:, k * width : (k + 1) * width], downs[k][...], preferred_element_type=jnp.float32
        )
        total = part if total is None else total + part
    answer = total.astype(jnp.bfloat16)
    height = answer.shape[0] // len(outs)
    for i, out in enumerate(outs):
        out[...] = answer[i * height : (i + 1) * height]


def combine_kernel(blocks, high_ref, low_ref, *refs):
    out_ref = refs[-1]
    rows = jnp.concatenate([r[...] for r in refs[:blocks]], axis=0)
    total = jnp.dot(high_ref[...], rows, preferred_element_type=jnp.float32)
    total = total + jnp.dot(low_ref[...], rows, preferred_element_type=jnp.float32)
    if len(refs) > blocks + 1:
        total = total + refs[blocks][...]
    out_ref[...] = total.astype(out_ref.dtype)


def mixer_a_kernel(rows_ref, gain_ref, value_ref, inner_ref, outer_ref, mixed_ref, gate_ref, top_ref, bottom_ref):
    wide = rows_ref[...].astype(jnp.float32)
    scale = lax.rsqrt(jnp.mean(wide * wide, axis=-1, keepdims=True) + EPSILON)
    norm = (wide * scale * gain_ref[...]).astype(jnp.bfloat16)
    value = jnp.dot(norm, value_ref[...], preferred_element_type=jnp.float32)
    inner = jnp.dot(norm, inner_ref[...], preferred_element_type=jnp.float32)
    gate_ref[...] = jnp.dot(norm, outer_ref[...], preferred_element_type=jnp.float32)
    mixed = inner * value
    mixed_ref[...] = mixed.astype(jnp.bfloat16)
    count = mixed.shape[0]

    @pl.when(pl.program_id(0) == 0)
    def _():
        top_ref[...] = mixed[:1].astype(jnp.bfloat16)

    @pl.when(pl.program_id(0) == pl.num_programs(0) - 1)
    def _():
        bottom_ref[...] = mixed[count - 1 :].astype(jnp.bfloat16)


def mixer_a(rows, gain, value_weight, inner_gate, outer_gate, steps):
    total, width = rows.shape
    channels = value_weight.shape[1]
    height = total // steps
    whole = pl.BlockSpec((width, channels), lambda i: (0, 0))
    edge = pl.BlockSpec((1, channels), lambda i: (0, 0))
    piece = pl.BlockSpec((height, channels), lambda i: (i, 0))
    return pl.pallas_call(
        mixer_a_kernel,
        grid=(steps,),
        out_shape=[
            jax.ShapeDtypeStruct((total, channels), jnp.bfloat16),
            jax.ShapeDtypeStruct((total, channels), jnp.float32),
            jax.ShapeDtypeStruct((1, channels), jnp.bfloat16),
            jax.ShapeDtypeStruct((1, channels), jnp.bfloat16),
        ],
        in_specs=[
            pl.BlockSpec((height, width), lambda i: (i, 0)),
            pl.BlockSpec((1, width), lambda i: (0, 0)),
            whole,
            whole,
            whole,
        ],
        out_specs=[piece, piece, edge, edge],
        name="mixer_a",
    )(rows, gain.reshape(1, width), value_weight, inner_gate, outer_gate)


def mixer_b_kernel(split, me_ref, mixed_ref, gate_ref, above_ref, below_ref, taps_ref, proj_ref, *refs):
    rows_ref = refs[-1]
    outs = refs[:-1]
    mixed = mixed_ref[...].astype(jnp.float32)
    count = mixed.shape[0]
    place = lax.broadcasted_iota(jnp.int32, mixed.shape, 0)
    before = jnp.where(place == 0, above_ref[...].astype(jnp.float32), pltpu.roll(mixed, 1, 0))
    after = jnp.where(place == count - 1, below_ref[...].astype(jnp.float32), pltpu.roll(mixed, count - 1, 0))
    summed = taps_ref[0:1, :] * before + taps_ref[1:2, :] * mixed + taps_ref[2:3, :] * after
    rows_ref[...] = (gate_ref[...] * summed).astype(jnp.bfloat16)
    owned = count // split
    for k, out in enumerate(outs):
        start = pl.multiple_of((me_ref[0] ^ k) * owned, owned)
        part = jnp.dot(rows_ref[pl.ds(start, owned), :], proj_ref[...], preferred_element_type=jnp.float32)
        out[...] = part.astype(out.dtype)


def add_kernel(*refs):
    total = refs[0][...].astype(jnp.float32)
    for ref in refs[1:-1]:
        total = total + ref[...].astype(jnp.float32)
    refs[-1][...] = total.astype(refs[-1].dtype)


def gathered_blocks(piece, axis):
    count = lax.axis_size(axis)
    blocks = [piece]
    for k in range(1, count):
        low = k & -k
        blocks.append(swapped(blocks[k ^ low], axis, low))
    return blocks


def on_device(
    mixer_input,
    mixer_gain,
    value_weight,
    inner_gate,
    outer_gate,
    kernel_taps,
    mixer_proj,
    expert_input,
    expert_gain,
    routes,
    group_logits,
    pair_logits,
    gate_weight,
    up_weight,
    down_weight,
):
    experts = lax.axis_size("ep")
    split = lax.axis_size("tp")
    local, width = expert_input.shape
    capacity = 4 * local // experts
    slots = experts * capacity
    direct = experts == 8
    height = capacity if direct else slots
    count = slots // height
    bf16, f32 = jnp.bfloat16, jnp.float32
    shaped = jax.ShapeDtypeStruct
    me_tp = lax.axis_index("tp").astype(jnp.int32).reshape(1)
    me_ep = lax.axis_index("ep").astype(jnp.int32)
    me_ep = (me_ep if direct else jnp.zeros((), jnp.int32)).reshape(1)

    gates = gathered_blocks(gate_weight[0], "tp")
    uppers = gathered_blocks(up_weight[0], "tp")
    downs = gathered_blocks(down_weight[0], "tp")

    outgoing = call(
        lambda *refs: dispatch_kernel(experts, capacity, *refs),
        [shaped((height, width), bf16)] * count,
        me_ep,
        expert_input,
        expert_gain.reshape(1, width),
        routes.T,
        smem=1,
    )

    def exchanged(value):
        rows = value.reshape(experts, capacity, width)
        return lax.all_to_all(rows, "ep", split_axis=0, concat_axis=0, tiled=True).reshape(slots, width)

    if direct:
        arrived = [outgoing[0]] + [swapped(outgoing[d], "ep", d) for d in range(1, count)]
        groups = (("near", range(0, 4)), ("far_b", range(6, 8)), ("far_a", range(4, 6)))
    else:
        arrived = [exchanged(outgoing[0])]
        groups = (("near", range(1)),)

    mixed, gate, top, bottom = mixer_a(mixer_input, mixer_gain, value_weight, inner_gate, outer_gate, split)
    last = experts - 1
    above = lax.ppermute(bottom, "ep", [(i, i + 1) for i in range(last)])
    below = lax.ppermute(top, "ep", [(i + 1, i) for i in range(last)])

    ordered = sorted(groups, key=lambda g: g[1][0])
    heights = [len(members) * height for _, members in ordered]
    shares = call(
        lambda *refs: share_kernel(experts, capacity, heights, *refs),
        [shaped((local, h), bf16) for h in heights for _ in range(2)],
        me_ep,
        routes.T,
        group_logits.T,
        pair_logits.T,
        smem=1,
    )
    shares = {name: shares[2 * i : 2 * i + 2] for i, (name, _) in enumerate(ordered)}

    back = {}
    units = split * gate_weight.shape[2]
    for name, members in groups:
        n = len(members)
        hidden = call(
            lambda *refs, n=n: hidden_kernel(n, split, *refs),
            shaped((n * height, units), bf16),
            *[arrived[d] for d in members],
            *gates,
            *uppers,
        )
        answers = call(lambda *refs: down_kernel(split, *refs), [shaped((height, width), bf16)] * n, hidden, *downs)
        for d, answer in zip(members, answers):
            if not direct:
                back[d] = exchanged(answer)
            else:
                back[d] = swapped(answer, "ep", d) if d else answer

    owned = mixed.shape[0] // split
    parts = call(
        lambda *refs: mixer_b_kernel(split, *refs),
        [shaped((owned, width), bf16 if k % 2 else f32) for k in range(split)],
        me_tp,
        mixed,
        gate,
        above,
        below,
        kernel_taps,
        mixer_proj,
        scratch=[pltpu.VMEM(mixed.shape, bf16)],
        smem=1,
    )
    addends = [[part] for part in parts]
    bit = 1
    while bit < split:
        for k in reversed(range(bit, split, 2 * bit)):
            value = addends[k][0]
            if bit > 1:
                value = call(add_kernel, shaped((owned, width), bf16), *addends[k])
            addends[k - bit].append(swapped(value, "tp", bit))
        bit *= 2
    mixer_output = call(add_kernel, shaped((owned, width), bf16), *addends[0])

    total = []
    for i, (name, members) in enumerate(groups):
        kind = bf16 if i == len(groups) - 1 else f32
        blocks = [back[d] for d in members]
        total = [
            call(
                lambda *refs, n=len(blocks): combine_kernel(n, *refs),
                shaped((local, width), kind),
                *shares[name],
                *blocks,
                *total,
            )
        ]
    return (mixer_output, total[0])


def solution(mesh):
    in_specs = (
        P("ep", None),
        P(),
        P(None, "tp"),
        P(None, "tp"),
        P(None, "tp"),
        P(None, "tp"),
        P("tp", None),
        P(("ep", "tp"), None),
        P(),
        P(("ep", "tp"), None),
        P(("ep", "tp"), None),
        P(("ep", "tp"), None),
        P("ep", None, "tp"),
        P("ep", None, "tp"),
        P("ep", "tp", None),
    )
    out_specs = (P(("ep", "tp"), None), P(("ep", "tp"), None))

    return jax.shard_map(on_device, mesh=mesh, in_specs=in_specs, out_specs=out_specs, check_vma=False)
```

```python
import jax
import jax.numpy as jnp
from jax import lax
from jax.experimental import pallas as pl
from jax.experimental.pallas import tpu as pltpu
from jax.sharding import PartitionSpec as P


EPG = 8
EPSILON = 1e-06
CHUNKS = 2


def swapped(value, axis, bit):
    count = lax.axis_size(axis)
    return lax.ppermute(value, axis, [(i, i ^ bit) for i in range(count)])


def call(body, outs, *operands, scratch=(), smem=0, limit=16, placed=True):
    vmem = pl.BlockSpec(memory_space=pltpu.VMEM)
    scalar = pl.BlockSpec(memory_space=pltpu.SMEM)
    near = operands[smem:]
    if placed:
        near = [pltpu.with_memory_space_constraint(x, pltpu.VMEM) for x in near]
    return pl.pallas_call(
        body,
        out_shape=[pltpu.VMEM(o.shape, o.dtype) for o in outs],
        in_specs=[scalar] * smem + [vmem] * len(near),
        out_specs=[vmem] * len(outs),
        scratch_shapes=list(scratch),
        compiler_params=pltpu.CompilerParams(vmem_limit_bytes=limit << 20),
    )(*operands[:smem], *near)


def slots_of(experts, capacity, me, routes_ref):
    first, second = routes_ref[0:1, :], routes_ref[1:2, :]
    local = first.shape[1]
    expert = lax.broadcasted_iota(jnp.int32, (experts, local), 0)
    hit_first = jnp.where(expert == first, 1.0, 0.0)
    hit_second = jnp.where(expert == second, 1.0, 0.0)
    row = lax.broadcasted_iota(jnp.int32, (local, local), 0)
    column = lax.broadcasted_iota(jnp.int32, (local, local), 1)
    earlier = jnp.where(row < column, 1.0, 0.0).astype(jnp.bfloat16)
    before_first = jnp.dot(hit_first.astype(jnp.bfloat16), earlier, preferred_element_type=jnp.float32)
    before_second = jnp.dot(hit_second.astype(jnp.bfloat16), earlier, preferred_element_type=jnp.float32)
    before_second = before_second + jnp.sum(hit_first, axis=1, keepdims=True)
    rank_first = jnp.sum(hit_first * before_first, axis=0, keepdims=True).astype(jnp.int32)
    rank_second = jnp.sum(hit_second * before_second, axis=0, keepdims=True).astype(jnp.int32)
    slot = lax.broadcasted_iota(jnp.int32, (experts * capacity, local), 0)
    is_first = slot == (first ^ me) * capacity + rank_first
    is_second = slot == (second ^ me) * capacity + rank_second
    return is_first, is_second


def dispatch_kernel(experts, capacity, me_ref, rows_ref, gain_ref, routes_ref, *blocks):
    is_first, is_second = slots_of(experts, capacity, me_ref[0], routes_ref)
    place = jnp.where(is_first | is_second, 1.0, 0.0).astype(jnp.bfloat16)
    wide = rows_ref[...].astype(jnp.float32)
    scale = lax.rsqrt(jnp.mean(wide * wide, axis=-1, keepdims=True) + EPSILON)
    norm = (wide * scale * gain_ref[...]).astype(jnp.bfloat16)
    placed = jnp.dot(place, norm, preferred_element_type=jnp.float32).astype(jnp.bfloat16)
    height = placed.shape[0] // len(blocks)
    for i, block in enumerate(blocks):
        block[...] = placed[i * height : (i + 1) * height]


def share_kernel(experts, capacity, heights, me_ref, routes_ref, group_ref, pair_ref, *outs):
    is_first, is_second = slots_of(experts, capacity, me_ref[0], routes_ref)
    logits = group_ref[...]
    first = routes_ref[0:1, :]
    group = lax.broadcasted_iota(jnp.int32, logits.shape, 0)
    chosen = (group * EPG <= first) & (first < group * EPG + EPG)
    picked = jnp.sum(jnp.where(chosen, logits, 0.0), axis=0, keepdims=True)
    group_weight = 1.0 / jnp.sum(jnp.exp(logits - picked), axis=0, keepdims=True)
    apart = pair_ref[0:1, :] - pair_ref[1:2, :]
    weight_first = group_weight / (1.0 + jnp.exp(-apart))
    weight_second = group_weight / (1.0 + jnp.exp(apart))
    weights = jnp.where(is_first, weight_first, 0.0) + jnp.where(is_second, weight_second, 0.0)
    start = 0
    for i, height in enumerate(heights):
        share = weights[start : start + height].T
        high = share.astype(jnp.bfloat16)
        outs[2 * i][...] = high
        outs[2 * i + 1][...] = (share - high.astype(jnp.float32)).astype(jnp.bfloat16)
        start += height


def hidden_kernel(blocks, split, *refs):
    out_ref = refs[-1]
    rows = jnp.concatenate([r[...] for r in refs[:blocks]], axis=0)
    gates = refs[blocks : blocks + split]
    uppers = refs[blocks + split : blocks + 2 * split]
    width = gates[0].shape[1]
    for k in range(split):
        first = jnp.dot(rows, gates[k][...], preferred_element_type=jnp.float32)
        second = jnp.dot(rows, uppers[k][...], preferred_element_type=jnp.float32)
        value = first / (1.0 + jnp.exp(-first)) * second
        out_ref[:, k * width : (k + 1) * width] = value.astype(jnp.bfloat16)


def down_kernel(split, *refs):
    hidden_ref = refs[0]
    downs = refs[1 : 1 + split]
    outs = refs[1 + split :]
    width = downs[0].shape[0]
    total = None
    for k in range(split):
        part = jnp.dot(
            hidden_ref[:, k * width : (k + 1) * width], downs[k][...], preferred_element_type=jnp.float32
        )
        total = part if total is None else total + part
    answer = total.astype(jnp.bfloat16)
    height = answer.shape[0] // len(outs)
    for i, out in enumerate(outs):
        out[...] = answer[i * height : (i + 1) * height]


def combine_kernel(blocks, total, *refs):
    out_ref = refs[-1]
    high_ref, low_ref = refs[:2]
    rows = jnp.concatenate([r[...] for r in refs[2 : 2 + blocks]], axis=0)
    value = jnp.dot(high_ref[...], rows, preferred_element_type=jnp.float32)
    value = value + jnp.dot(low_ref[...], rows, preferred_element_type=jnp.float32)
    others = refs[2 + blocks : -1]
    if total:
        value = value + others[0][...]
        others = others[1:]
    start = 0
    for done in others:
        out_ref[:, start : start + done.shape[1]] = done[...]
        start += done.shape[1]
    out_ref[:, start:] = value.astype(out_ref.dtype)


def mixer_a_kernel(rows_ref, gain_ref, value_ref, inner_ref, outer_ref, mixed_ref, gate_ref, top_ref, bottom_ref):
    wide = rows_ref[...].astype(jnp.float32)
    scale = lax.rsqrt(jnp.mean(wide * wide, axis=-1, keepdims=True) + EPSILON)
    norm = (wide * scale * gain_ref[...]).astype(jnp.bfloat16)
    value = jnp.dot(norm, value_ref[...], preferred_element_type=jnp.float32)
    inner = jnp.dot(norm, inner_ref[...], preferred_element_type=jnp.float32)
    gate_ref[...] = jnp.dot(norm, outer_ref[...], preferred_element_type=jnp.float32)
    mixed = inner * value
    mixed_ref[...] = mixed.astype(jnp.bfloat16)
    count = mixed.shape[0]

    @pl.when(pl.program_id(0) == 0)
    def _():
        top_ref[...] = mixed[:1].astype(jnp.bfloat16)

    @pl.when(pl.program_id(0) == pl.num_programs(0) - 1)
    def _():
        bottom_ref[...] = mixed[count - 1 :].astype(jnp.bfloat16)


def mixer_a(rows, gain, value_weight, inner_gate, outer_gate, steps):
    total, width = rows.shape
    channels = value_weight.shape[1]
    height = total // steps
    whole = pl.BlockSpec((width, channels), lambda i: (0, 0))
    edge = pl.BlockSpec((1, channels), lambda i: (0, 0))
    piece = pl.BlockSpec((height, channels), lambda i: (i, 0))
    return pl.pallas_call(
        mixer_a_kernel,
        grid=(steps,),
        out_shape=[
            jax.ShapeDtypeStruct((total, channels), jnp.bfloat16),
            jax.ShapeDtypeStruct((total, channels), jnp.float32),
            jax.ShapeDtypeStruct((1, channels), jnp.bfloat16),
            jax.ShapeDtypeStruct((1, channels), jnp.bfloat16),
        ],
        in_specs=[
            pl.BlockSpec((height, width), lambda i: (i, 0)),
            pl.BlockSpec((1, width), lambda i: (0, 0)),
            whole,
            whole,
            whole,
        ],
        out_specs=[piece, piece, edge, edge],
        name="MA",
    )(rows, gain.reshape(1, width), value_weight, inner_gate, outer_gate)


def mixer_b_kernel(split, me_ref, mixed_ref, gate_ref, above_ref, below_ref, taps_ref, proj_ref, *refs):
    rows_ref = refs[-1]
    outs = refs[:-1]
    mixed = mixed_ref[...].astype(jnp.float32)
    count = mixed.shape[0]
    place = lax.broadcasted_iota(jnp.int32, mixed.shape, 0)
    before = jnp.where(place == 0, above_ref[...].astype(jnp.float32), pltpu.roll(mixed, 1, 0))
    after = jnp.where(place == count - 1, below_ref[...].astype(jnp.float32), pltpu.roll(mixed, count - 1, 0))
    summed = taps_ref[0:1, :] * before + taps_ref[1:2, :] * mixed + taps_ref[2:3, :] * after
    rows_ref[...] = (gate_ref[...] * summed).astype(jnp.bfloat16)
    owned = count // split
    for k, out in enumerate(outs):
        start = pl.multiple_of((me_ref[0] ^ k) * owned, owned)
        part = jnp.dot(rows_ref[pl.ds(start, owned), :], proj_ref[...], preferred_element_type=jnp.float32)
        out[...] = part.astype(out.dtype)


def add_kernel(*refs):
    total = refs[0][...].astype(jnp.float32)
    for ref in refs[1:-1]:
        total = total + ref[...].astype(jnp.float32)
    refs[-1][...] = total.astype(refs[-1].dtype)


def gathered_blocks(piece, axis):
    count = lax.axis_size(axis)
    blocks = [piece]
    for k in range(1, count):
        low = k & -k
        blocks.append(swapped(blocks[k ^ low], axis, low))
    return blocks


def on_device(
    mixer_input,
    mixer_gain,
    value_weight,
    inner_gate,
    outer_gate,
    kernel_taps,
    mixer_proj,
    expert_input,
    expert_gain,
    routes,
    group_logits,
    pair_logits,
    gate_weight,
    up_weight,
    down_weight,
):
    experts = lax.axis_size("ep")
    split = lax.axis_size("tp")
    local, width = expert_input.shape
    capacity = 4 * local // experts
    slots = experts * capacity
    direct = experts == 8
    height = capacity if direct else slots
    count = slots // height
    bf16, f32 = jnp.bfloat16, jnp.float32
    shaped = jax.ShapeDtypeStruct
    me_tp = lax.axis_index("tp").astype(jnp.int32).reshape(1)
    me_ep = lax.axis_index("ep").astype(jnp.int32)
    me_ep = (me_ep if direct else jnp.zeros((), jnp.int32)).reshape(1)

    gates = gathered_blocks(gate_weight[0], "tp")
    uppers = gathered_blocks(up_weight[0], "tp")
    column = width // CHUNKS
    cut = [down_weight[0][:, c * column : (c + 1) * column] for c in range(CHUNKS)]
    downs = [gathered_blocks(cut[c], "tp") for c in range(CHUNKS)]

    outgoing = call(
        lambda *refs: dispatch_kernel(experts, capacity, *refs),
        [shaped((height, width), bf16)] * count,
        me_ep,
        expert_input,
        expert_gain.reshape(1, width),
        routes.T,
        smem=1,
        placed=False,
    )

    def exchanged(value):
        rows = value.reshape(experts, capacity, value.shape[1])
        rows = lax.all_to_all(rows, "ep", split_axis=0, concat_axis=0, tiled=True)
        return rows.reshape(slots, value.shape[1])

    if direct:
        arrived = [outgoing[0]] + [swapped(outgoing[d], "ep", d) for d in range(1, count)]
        groups = (("N", range(0, 4)), ("B", range(6, 8)), ("A", range(4, 6)))
    else:
        arrived = [exchanged(outgoing[0])]
        groups = (("N", range(1)),)

    mixed, gate, top, bottom = mixer_a(mixer_input, mixer_gain, value_weight, inner_gate, outer_gate, split)
    last = experts - 1
    above = lax.ppermute(bottom, "ep", [(i, i + 1) for i in range(last)])
    below = lax.ppermute(top, "ep", [(i + 1, i) for i in range(last)])

    ordered = sorted(groups, key=lambda g: g[1][0])
    heights = [len(members) * height for _, members in ordered]
    shares = call(
        lambda *refs: share_kernel(experts, capacity, heights, *refs),
        [shaped((local, h), bf16) for h in heights for _ in range(2)],
        me_ep,
        routes.T,
        group_logits.T,
        pair_logits.T,
        smem=1,
    )
    shares = {name: shares[2 * i : 2 * i + 2] for i, (name, _) in enumerate(ordered)}

    back = [{} for _ in range(CHUNKS)]
    units = split * gate_weight.shape[2]
    hiddens = {}
    for name, members in groups:
        n = len(members)
        (hiddens[name],) = call(
            lambda *refs, n=n: hidden_kernel(n, split, *refs),
            [shaped((n * height, units), bf16)],
            *[arrived[d] for d in members],
            *gates,
            *uppers,
        )
    for c in range(CHUNKS):
        for name, members in groups:
            answers = call(
                lambda *refs: down_kernel(split, *refs),
                [shaped((height, column), bf16)] * len(members),
                hiddens[name],
                *downs[c],
            )
            for d, answer in zip(members, answers):
                if not direct:
                    back[c][d] = exchanged(answer)
                else:
                    back[c][d] = swapped(answer, "ep", d) if d else answer

    owned = mixed.shape[0] // split
    parts = call(
        lambda *refs: mixer_b_kernel(split, *refs),
        [shaped((owned, width), bf16 if k % 2 else f32) for k in range(split)],
        me_tp,
        mixed,
        gate,
        above,
        below,
        kernel_taps,
        mixer_proj,
        scratch=[pltpu.VMEM(mixed.shape, bf16)],
        smem=1,
    )
    addends = [[part] for part in parts]
    bit = 1
    while bit < split:
        for k in reversed(range(bit, split, 2 * bit)):
            value = addends[k][0]
            if bit > 1:
                (value,) = call(add_kernel, [shaped((owned, width), bf16)], *addends[k])
            addends[k - bit].append(swapped(value, "tp", bit))
        bit *= 2
    (mixer_output,) = call(add_kernel, [shaped((owned, width), bf16)], *addends[0])

    finished = []
    for c in range(CHUNKS):
        total = []
        for i, (name, members) in enumerate(groups):
            last = i == len(groups) - 1
            before = finished if last and c == CHUNKS - 1 else []
            blocks = [back[c][d] for d in members]
            total = call(
                lambda *refs, n=len(blocks), t=len(total): combine_kernel(n, t, *refs),
                [shaped((local, column * (1 + len(before))), bf16 if last else f32)],
                *shares[name],
                *blocks,
                *total,
                *before,
            )
        finished = finished + list(total)
    return (mixer_output, finished[-1])


def solution(mesh):
    in_specs = (
        P("ep", None),
        P(),
        P(None, "tp"),
        P(None, "tp"),
        P(None, "tp"),
        P(None, "tp"),
        P("tp", None),
        P(("ep", "tp"), None),
        P(),
        P(("ep", "tp"), None),
        P(("ep", "tp"), None),
        P(("ep", "tp"), None),
        P("ep", None, "tp"),
        P("ep", None, "tp"),
        P("ep", "tp", None),
    )
    out_specs = (P(("ep", "tp"), None), P(("ep", "tp"), None))

    return jax.shard_map(on_device, mesh=mesh, in_specs=in_specs, out_specs=out_specs, check_vma=False)
```
